512 devices in a mesh: dp: 4 (over x), kv: 64 (over z, y), tp: 2 (over core).
Axes of the slice: x: 4, y: 8, z: 8, core: 2. Of those that a mesh axis runs over, the one named last changes fastest.
Arguments:
- tokens: bfloat16 [32, 1024], P('dp', 'kv'), may hold values from -6 to 6
- norm_gain: float32 [1024], P('kv'), may hold values from 0.1 to 1.9
- w_query: bfloat16 [1024, 4, 64], P('kv', 'tp'), may hold values from -0.1875 to 0.1875
- w_key: bfloat16 [1024, 4, 64], P('kv', 'tp'), may hold values from -0.1875 to 0.1875
- w_value: bfloat16 [1024, 4, 64], P('kv', 'tp'), may hold values from -0.1875 to 0.1875
- w_gate: bfloat16 [1024, 4, 64], P('kv', 'tp'), may hold values from -0.1875 to 0.1875
- w_forget: bfloat16 [1024, 4], P('kv', 'tp'), may hold values from -0.1875 to 0.1875
- w_out: bfloat16 [4, 64, 1024], P('tp', None, 'kv'), may hold values from -0.375 to 0.375
- cache_key: bfloat16 [32, 32768, 4, 64], P('dp', 'kv', 'tp'), may hold values from -6 to 6
- cache_value: bfloat16 [32, 32768, 4, 64], P('dp', 'kv', 'tp'), may hold values from -6 to 6
- cache_logf: float32 [32, 32768, 4], P('dp', 'kv', 'tp'), may hold values from -0.60003052 to 0, as said below
- lengths: int32 [32], P('dp'), may hold values from 31744 to 32767
Outputs:
- mixed: float32 [32, 1024], P('dp', 'kv')
- new_key: bfloat16 [32, 4, 64], P('dp', 'tp')
- new_value: float32 [32, 4, 64], P('dp', 'tp')
- new_logf: float32 [32, 4], P('dp', 'tp')
The draws below stay inside these ranges and needn't reach their ends.
Inputs may be any that keep to these rules, and one draw needn't show every extreme that they name: `lengths`: each sequence has between 31744 and 32767 cached tokens. `cache_logf`: log forget gates are at most 0; most are small (down to -1 / 32768, with a typical size that differs by head), and about six positions of each sequence and head hold drops of 0.2 to 0.6.
All inputs are finite; a program needn't handle non-finite values.
Results may differ from the reference program's by a relative error of at most 0.0095.
Values sent between devices are 32-bit elements.
No kernel may reach another device: no remote copies, remote signals or barrier semaphores. Data moves between devices by JAX's collectives and lax.ppermute only.
A program may use at most 64 MiB of HBM per device.

```python
import math
import jax
import jax.numpy as jnp
from jax import lax

D = 1024
HEADS = 4
HEAD_DIM = 64
POS_DEV = 512
BATCH = 32
CTX = 32768


def draw_cache_logf(key, part):
    rate_key, spread_key, spike_key, height_key = jax.random.split(key, 4)
    head_rates = jnp.exp(jax.random.uniform(rate_key, (HEADS,), jnp.float32, math.log(0.05), math.log(0.5)))
    spread = jax.random.uniform(spread_key, (BATCH, CTX, HEADS), jnp.float32, 0.0, 2.0)
    spike_mask = jax.random.bernoulli(spike_key, 6.0 / CTX, (BATCH, CTX, HEADS))
    heights = jax.random.uniform(height_key, (BATCH, CTX, HEADS), jnp.float32, 0.2, 0.6)
    return -(spread * head_rates[None, None, :] / CTX) - jnp.where(spike_mask, heights, jnp.float32(0.0))


def place_ends(drawn, own_key, smallest, top_value):
    spot = [jax.random.randint(jax.random.fold_in(own_key, axis), (), 0, length) for axis, length in enumerate(drawn.shape)]
    main_axis = drawn.shape.index(max(drawn.shape))
    next_to = spot[:main_axis] + [(spot[main_axis] + 1) % drawn.shape[main_axis]] + spot[main_axis + 1:]
    return drawn.at[tuple(spot)].set(smallest).at[tuple(next_to)].set(top_value)


def shard_levels(rng, dims, cuts, least, top_value):
    level = 1.0
    for dim, shards_of in cuts:
        steps = jax.random.uniform(jax.random.fold_in(jax.random.fold_in(rng, 6), dim), (shards_of,), jnp.float32, least / len(cuts), top_value / len(cuts))
        level = level * jnp.repeat(jnp.exp(steps), dims[dim] // shards_of).reshape((-1,) + (1,) * (len(dims) - 1 - dim))
    return level


def noise(rng, shape, deviation, limit, cuts=(), kind=jnp.bfloat16):
    factor_of = shard_levels(rng, shape, cuts, -0.22, 0.18) if cuts else 1.0
    drawn = jax.random.normal(rng, shape, jnp.float32) * deviation * factor_of
    return jnp.minimum(jnp.maximum(drawn, -limit), limit).astype(kind)


def setup_inputs(seed: int = 0) -> dict:
    arg_keys = jax.random.split(jax.random.key(seed), 13)
    tokens = noise(arg_keys[0], (BATCH, D), 1.0, 6.0, ((0, 4), (1, 64)))
    norm_gain = jnp.clip(1.0 + 0.18 * jax.random.normal(arg_keys[1], (D,), jnp.float32), 0.1, 1.9)
    w_query = noise(arg_keys[2], (D, HEADS, HEAD_DIM), D ** -0.5, 0.1875, ((0, 64), (1, 2)))
    w_key = noise(arg_keys[3], (D, HEADS, HEAD_DIM), D ** -0.5, 0.1875, ((0, 64), (1, 2)))
    w_value = noise(arg_keys[4], (D, HEADS, HEAD_DIM), D ** -0.5, 0.1875, ((0, 64), (1, 2)))
    w_gate = noise(arg_keys[5], (D, HEADS, HEAD_DIM), D ** -0.5, 0.1875, ((0, 64), (1, 2)))
    w_forget = noise(arg_keys[6], (D, HEADS), D ** -0.5, 0.1875, ((0, 64), (1, 2)))
    w_out = noise(arg_keys[7], (HEADS, HEAD_DIM, D), (HEADS * HEAD_DIM) ** -0.5, 0.375, ((0, 2), (2, 64)))
    cache_key = noise(arg_keys[8], (BATCH, CTX, HEADS, HEAD_DIM), 1.0, 6.0, ((0, 4), (1, 64), (2, 2)))
    cache_value = noise(arg_keys[9], (BATCH, CTX, HEADS, HEAD_DIM), 1.0, 6.0, ((0, 4), (1, 64), (2, 2)))
    cache_logf = draw_cache_logf(jax.random.fold_in(arg_keys[12], 71), 0)
    lengths = place_ends(jax.random.randint(arg_keys[11], (BATCH,), CTX - 2 * POS_DEV, CTX), jax.random.fold_in(arg_keys[11], 1), CTX - 2 * POS_DEV, CTX - 1).astype(jnp.int32)
    return dict(tokens=tokens, norm_gain=norm_gain, w_query=w_query, w_key=w_key, w_value=w_value, w_gate=w_gate, w_forget=w_forget, w_out=w_out, cache_key=cache_key, cache_value=cache_value, cache_logf=cache_logf, lengths=lengths)


eps = 1e-06
very_low = -1e+30

def head_norm(values):
    return values * lax.rsqrt(lax.optimization_barrier(jnp.mean(values * values, axis=-1, keepdims=True)) + eps)

def one_sequence(packed):
    query_vec, key_new, value_new, logf_new, keys_all, values_all, logf_all, length = packed
    positions = jnp.arange(keys_all.shape[0], dtype=jnp.int32)
    in_range = positions < length
    masked_logf = jnp.where(in_range[:, None], logf_all, jnp.float32(0.0))
    running = jnp.cumsum(masked_logf, axis=0)
    later_sum = running[-1][None, :] - running
    forget_bias = logf_new[None, :] + later_sum
    wide_query = query_vec.astype(jnp.float32)
    scores = jnp.einsum('he,she->hs', wide_query, keys_all.astype(jnp.float32)) * HEAD_DIM ** (-0.5) + forget_bias.T
    score_new = lax.optimization_barrier(jnp.sum(wide_query * key_new.astype(jnp.float32), axis=-1)) * HEAD_DIM ** (-0.5)
    peak = jnp.maximum(lax.optimization_barrier(jnp.max(jnp.where(in_range[None, :], scores, very_low), axis=-1)), score_new)
    weights = jnp.where(in_range[None, :], jnp.exp(scores - peak[:, None]), jnp.float32(0.0))
    weight_new = jnp.exp(score_new - peak)
    denominator = lax.optimization_barrier(jnp.sum(weights, axis=-1)) + weight_new
    weighted = jnp.einsum('hs,she->he', weights.astype(jnp.bfloat16).astype(jnp.float32), values_all.astype(jnp.float32))
    weighted = weighted + weight_new[:, None] * value_new
    return weighted / denominator[:, None]

def reference(tokens, norm_gain, w_query, w_key, w_value, w_gate, w_forget, w_out, cache_key, cache_value, cache_logf, lengths):
    wide_tokens = tokens.astype(jnp.float32)
    inv_root = lax.rsqrt(lax.optimization_barrier(jnp.mean(wide_tokens * wide_tokens, axis=-1, keepdims=True)) + eps)
    normed = (wide_tokens * inv_root * norm_gain).astype(jnp.bfloat16)
    wide_normed = normed.astype(jnp.float32)

    def project(weight):
        return jnp.einsum('bd,dhe->bhe', wide_normed, weight.astype(jnp.float32))
    query_vec = head_norm(project(w_query)).astype(jnp.bfloat16)
    key_new = head_norm(project(w_key)).astype(jnp.bfloat16)
    value_new = project(w_value)
    gate_silu = jax.nn.silu(project(w_gate))
    logf_new = jax.nn.log_sigmoid(jnp.dot(normed, w_forget, preferred_element_type=jnp.float32))
    attended = lax.map(one_sequence, (query_vec, key_new, value_new, logf_new, cache_key, cache_value, cache_logf, lengths))
    gated = (head_norm(attended) * gate_silu).astype(jnp.bfloat16)
    mixed = jnp.einsum('bhe,hed->bd', gated.astype(jnp.float32), w_out.astype(jnp.float32))
    return (mixed, key_new, value_new, logf_new)
```

```python
import jax
import jax.numpy as jnp
from jax import lax
from jax.sharding import Mesh
from jax.sharding import PartitionSpec as P

D = 1024
HEAD_DIM = 64
KV = ("kv_0", "kv_1")
N_KV = 64

eps = 1e-06
very_low = -1e30
HI = lax.Precision.HIGHEST


def head_norm(values):
    return values * lax.rsqrt(jnp.mean(values * values, axis=-1, keepdims=True) + eps)


def exchange(slots):
    return lax.all_to_all(slots, KV, 0, 0, tiled=True)


def on_device(
    tokens,
    norm_gain,
    w_query,
    w_key,
    w_value,
    w_gate,
    w_forget,
    w_out,
    cache_key,
    cache_value,
    cache_logf,
    lengths,
):
    seqs, heads = tokens.shape[0], w_query.shape[1]
    wide_tokens = tokens.astype(jnp.float32)
    local_squares = jnp.sum(wide_tokens * wide_tokens, axis=1)
    scaled = wide_tokens * norm_gain

    def project(weight):
        return jnp.dot(
            scaled, weight.reshape(weight.shape[0], -1).astype(jnp.float32), precision=HI
        )

    part_query, part_key, part_value, part_gate = map(project, (w_query, w_key, w_value, w_gate))
    part_forget = project(w_forget)

    span = cache_key.shape[1]
    shard_index = lax.axis_index(KV)
    positions = shard_index * span + jnp.arange(span, dtype=jnp.int32)
    in_range = positions[None, :] < lengths[:, None]
    masked_logf = jnp.where(in_range[:, :, None], cache_logf, jnp.float32(0.0))
    shard_total = jnp.sum(masked_logf, axis=1)

    def spread(row):
        return jnp.broadcast_to(row.reshape(1, -1), (N_KV, row.size))

    pieces = [p.reshape(N_KV, -1) for p in (part_key, part_value, part_gate)]
    tail = [spread(local_squares), spread(part_forget), spread(shard_total)] + pieces
    tail = jnp.concatenate(tail, axis=1)
    tail = jnp.pad(tail, ((0, 0), (0, 128 - tail.shape[1])))
    first = jnp.concatenate(
        [jnp.broadcast_to(part_query[None], (N_KV, seqs, 128)), tail[:, None, :]], axis=1
    )
    first = exchange(first)
    summed = jnp.sum(first, axis=0)
    raw_query = summed[:seqs].reshape(seqs, heads, HEAD_DIM)
    sums = summed[seqs]
    inv_root = lax.rsqrt(sums[:seqs] / D + eps)
    forget = sums[seqs : seqs + 16].reshape(seqs, heads) * inv_root[:, None]
    logf_new = jax.nn.log_sigmoid(forget)
    totals = first[:, seqs, 24:40].reshape(N_KV, seqs, heads)
    own_pieces = sums[40:88]
    query_vec = head_norm(raw_query * inv_root[:, None, None]).astype(jnp.bfloat16)

    upper = (
        jnp.arange(span, dtype=jnp.int32)[:, None] > jnp.arange(span, dtype=jnp.int32)[None, :]
    ).astype(jnp.float32)
    later_inside = jnp.einsum("sph,pt->sht", masked_logf, upper, precision=HI)
    scores = jnp.einsum(
        "she,sphe->shp", query_vec, cache_key, preferred_element_type=jnp.float32
    ) * HEAD_DIM ** (-0.5)
    scores = scores + later_inside
    range_mask = in_range[:, None, :]
    local_peak = jnp.max(jnp.where(range_mask, scores, very_low), axis=-1)
    weights = jnp.where(range_mask, jnp.exp(scores - local_peak[..., None]), jnp.float32(0.0))
    local_den = jnp.sum(weights, axis=-1)
    local_sum = jnp.einsum(
        "shp,sphe->she",
        weights.astype(jnp.bfloat16),
        cache_value,
        preferred_element_type=jnp.float32,
    )

    row = jnp.concatenate([local_den.reshape(-1), local_peak.reshape(-1), own_pieces])
    row = jnp.pad(row, (0, 128 - row.shape[0]))
    second = jnp.concatenate([local_sum.reshape(seqs, 128), row[None]], axis=0)
    second = exchange(jnp.broadcast_to(second[None], (N_KV, seqs + 1, 128)))

    later = (
        jnp.arange(N_KV, dtype=jnp.int32)[None, :] > jnp.arange(N_KV, dtype=jnp.int32)[:, None]
    ).astype(jnp.float32)
    later_outside = jnp.einsum("ij,jsh->ish", later, totals, precision=HI)

    back = second[:, seqs]
    whole_key, whole_value, whole_gate = (
        back[:, 32 + 16 * n : 48 + 16 * n].reshape(seqs, heads, HEAD_DIM)
        * inv_root[:, None, None]
        for n in range(3)
    )
    key_new = head_norm(whole_key).astype(jnp.bfloat16)
    value_new = whole_value
    gate_silu = jax.nn.silu(whole_gate)
    score_new = jnp.sum(
        query_vec.astype(jnp.float32) * key_new.astype(jnp.float32), axis=-1
    ) * HEAD_DIM ** (-0.5)
    dens = back[:, :16].reshape(N_KV, seqs, heads)
    peaks = back[:, 16:32].reshape(N_KV, seqs, heads) + later_outside + logf_new[None]
    peak = jnp.maximum(jnp.max(peaks, axis=0), score_new)
    factors = jnp.exp(peaks - peak[None])
    weight_new = jnp.exp(score_new - peak)
    denominator = jnp.sum(factors * dens, axis=0) + weight_new
    parts = second[:, :seqs].reshape(N_KV, seqs, heads, HEAD_DIM)
    weighted = jnp.sum(factors[..., None] * parts, axis=0) + weight_new[..., None] * value_new
    attended = weighted / denominator[..., None]
    gated = (head_norm(attended) * gate_silu).astype(jnp.bfloat16)
    partial_out = jnp.einsum("she,hed->sd", gated, w_out, preferred_element_type=jnp.float32)
    mixed = lax.all_gather(partial_out, "tp").sum(0)
    return (mixed, key_new, value_new, logf_new)


def solution(mesh):
    finer = Mesh(
        mesh.devices.reshape(mesh.shape["dp"], 8, 8, mesh.shape["tp"]), ("dp", "kv_0", "kv_1", "tp")
    )
    return jax.shard_map(
        on_device,
        mesh=finer,
        in_specs=(
            P("dp", KV),
            P(KV),
            P(KV, "tp", None),
            P(KV, "tp", None),
            P(KV, "tp", None),
            P(KV, "tp", None),
            P(KV, "tp"),
            P("tp", None, KV),
            P("dp", KV, "tp", None),
            P("dp", KV, "tp", None),
            P("dp", KV, "tp"),
            P("dp"),
        ),
        out_specs=(P("dp", KV), P("dp", "tp", None), P("dp", "tp", None), P("dp", "tp")),
        check_vma=False,
    )
```

```python
import jax
import jax.numpy as jnp
from jax import lax
from jax.experimental import pallas as pl
from jax.experimental.pallas import tpu as pltpu
from jax.sharding import Mesh
from jax.sharding import PartitionSpec as P

D = 1024
HEAD_DIM = 64
KV = ("kv_0", "kv_1")
N_KV = 64
SEQS = 8
ROWS = 9
VMEM = 16 * 2**20
SPAN = 512
LANES = 128

eps = 1e-06
very_low = -1e30
HI = lax.Precision.HIGHEST
F32 = jnp.float32
NT = (((1,), (1,)), ((), ()))

FORGET, TOTAL, PIECES, PIECE = 8, 24, 40, 16


def iota(shape, dim):
    return lax.broadcasted_iota(jnp.int32, shape, dim)


def to_row(column, start):
    shape = (SEQS, LANES)
    picked = jnp.where(iota(shape, 1) == iota(shape, 0) + start, column, F32(0.0))
    return jnp.sum(picked, axis=0, keepdims=True)


def to_column(row, start):
    shape = (SEQS, LANES)
    picked = jnp.where(iota(shape, 1) == iota(shape, 0) + start, row, F32(0.0))
    return jnp.sum(picked, axis=1, keepdims=True)


def first_head():
    return iota((SEQS, LANES), 1) < HEAD_DIM


def per_head(values):
    low = jnp.sum(jnp.where(first_head(), values, F32(0.0)), axis=1, keepdims=True)
    high = jnp.sum(jnp.where(first_head(), F32(0.0), values), axis=1, keepdims=True)
    return low, high


def head_norm(values):
    low, high = per_head(values * values)
    return values * lax.rsqrt(jnp.where(first_head(), low, high) * (1.0 / HEAD_DIM) + eps)


def between(start, width):
    lane = iota((SEQS, LANES), 1)
    return (lane >= start) & (lane < start + width)


def row_of_slot(width):
    i = iota((1, width), 1)
    slot = (i * 7282) >> 16
    return slot, i - ROWS * slot


def prep(tokens, gain, w_query, w_key, w_value, w_gate, w_forget, logf, limits, slots):
    wide = tokens[...].astype(F32)
    squares = jnp.sum(wide * wide, axis=1, keepdims=True)
    scaled = wide * gain[...]

    def project(weight):
        return jnp.dot(scaled, weight[...].astype(F32), precision=HI, preferred_element_type=F32)

    forget = lax.dot_general(
        scaled, w_forget[...].astype(F32), NT, precision=HI, preferred_element_type=F32
    )
    live = iota((SEQS, SPAN), 1) < limits[...]
    row = to_row(squares, 0)
    for h in range(2):
        total = jnp.sum(jnp.where(live, logf[h], F32(0.0)), axis=1, keepdims=True)
        row = row + to_row(forget[:, h : h + 1], FORGET + SEQS * h)
        row = row + to_row(total, TOTAL + SEQS * h)
    query = project(w_query)
    parts = [project(w) for w in (w_key, w_value, w_gate)]
    for j in range(N_KV):
        slots[pl.ds(ROWS * j, SEQS), :] = query
    for c in range(8):
        tail = jnp.broadcast_to(row, (SEQS, LANES))
        for n, part in enumerate(parts):
            start = PIECES + PIECE * n
            moved = pltpu.roll(part, (start - PIECE * c) % LANES, 1)
            tail = jnp.where(between(start, PIECE), moved, tail)
        slots[pl.ds(ROWS * c + SEQS, SEQS, stride=ROWS * 8), :] = tail


def attend(slots, cache_key, cache_value, logf, limits, send, query_out, sums_out, shift_out):
    got = slots[...]
    width = N_KV * ROWS
    _, inside = row_of_slot(width)
    picks = (jnp.broadcast_to(inside, (16, width)) == iota((16, width), 0)).astype(F32)
    summed = jnp.dot(picks, got, precision=HI, preferred_element_type=F32)
    raw = summed[:SEQS]
    sums = summed[SEQS : SEQS + 1]
    inv_root = lax.rsqrt(to_column(sums, 0) * (1.0 / D) + eps)
    query = head_norm(raw * inv_root).astype(jnp.bfloat16)
    query_out[...] = query.astype(F32)
    sums_out[...] = jnp.broadcast_to(sums, (SEQS, LANES))

    tails = slots[pl.ds(SEQS, N_KV, stride=ROWS), :]
    shape = (N_KV, N_KV)
    upper = (iota(shape, 1) > iota(shape, 0)).astype(F32)
    shift_out[...] = jnp.dot(upper, tails, precision=HI, preferred_element_type=F32)

    blocks = []
    wide_query = query.astype(F32)
    seq = iota((SEQS, LANES), 0)
    for s in range(SEQS):
        mine = jnp.where(seq == s, wide_query, F32(0.0))
        low = jnp.where(first_head(), mine, F32(0.0))
        blocks.append(jnp.concatenate([low, mine - low], axis=0))
    spread = jnp.concatenate(blocks, axis=1).astype(jnp.bfloat16)
    keys = cache_key[...].reshape(SEQS * LANES, SPAN)
    scores = jnp.dot(spread, keys, preferred_element_type=F32) * HEAD_DIM ** (-0.5)

    live = iota((SEQS, SPAN), 1) < limits[...]
    live = jnp.concatenate([live.astype(F32), live.astype(F32)], axis=0) > 0.5
    gates = jnp.where(live, jnp.concatenate([logf[0], logf[1]], axis=0), F32(0.0))
    shape = (LANES, LANES)
    upper = (iota(shape, 0) > iota(shape, 1)).astype(F32)
    biases, after = [], jnp.zeros((2 * SEQS, 1), F32)
    for b in reversed(range(SPAN // LANES)):
        part = gates[:, LANES * b : LANES * (b + 1)]
        biases.append(jnp.dot(part, upper, precision=HI, preferred_element_type=F32) + after)
        after = after + jnp.sum(part, axis=1, keepdims=True)
    scores = scores + jnp.concatenate(biases[::-1], axis=1)
    peak = jnp.max(jnp.where(live, scores, F32(very_low)), axis=1, keepdims=True)
    weights = jnp.where(live, jnp.exp(scores - peak), F32(0.0))
    den = jnp.sum(weights, axis=1, keepdims=True)
    values = cache_value[...].reshape(SEQS * LANES, SPAN)
    crossed = lax.dot_general(
        weights.astype(jnp.bfloat16), values, NT, preferred_element_type=F32
    )
    local = jnp.zeros((SEQS, LANES), F32)
    for s in range(SEQS):
        block = crossed[:, LANES * s : LANES * (s + 1)]
        own = jnp.where(first_head(), block[:SEQS], block[SEQS:])
        local = jnp.where(seq == s, own, local)
    lane = iota((1, LANES), 1)
    row = jnp.where((lane >= PIECES) & (lane < PIECES + 3 * PIECE), sums, F32(0.0))
    for h in range(2):
        rows = slice(SEQS * h, SEQS * (h + 1))
        row = row + to_row(den[rows], SEQS * h) + to_row(peak[rows], TOTAL + SEQS * h)
    tail = jnp.broadcast_to(row, (SEQS, LANES))
    for j in range(N_KV):
        send[pl.ds(ROWS * j, SEQS), :] = local
    for c in range(8):
        send[pl.ds(ROWS * c + SEQS, SEQS, stride=ROWS * 8), :] = tail


def combine(slots, query, sums, shift, w_out, partial_out, key_out, value_out, logf_out):
    sums_row = sums[0:1, :]
    inv_root = lax.rsqrt(to_column(sums_row, 0) * (1.0 / D) + eps)
    parts = [jnp.zeros((SEQS, LANES), F32) for _ in range(3)]
    for c in range(8):
        tail = slots[pl.ds(ROWS * c + SEQS, SEQS, stride=ROWS * 8), :]
        for n in range(3):
            start = PIECES + PIECE * n
            moved = pltpu.roll(tail, (PIECE * c - start) % LANES, 1)
            parts[n] = jnp.where(between(PIECE * c, PIECE), moved, parts[n])
    key, value, gate = (part * inv_root for part in parts)
    key = head_norm(key).astype(jnp.bfloat16)
    key_out[...] = key
    value_out[...] = value
    score_new = [x * HEAD_DIM ** (-0.5) for x in per_head(query[...] * key.astype(F32))]
    tails = slots[pl.ds(SEQS, N_KV, stride=ROWS), :]
    logf_row = jnp.zeros((1, LANES), F32)
    score_row = jnp.zeros((1, LANES), F32)
    for h in range(2):
        forget = to_column(sums_row, FORGET + SEQS * h) * inv_root
        logf = jnp.minimum(forget, 0.0) - jnp.log1p(jnp.exp(-jnp.abs(forget)))
        logf_out[h] = jnp.broadcast_to(logf, (SEQS, LANES))
        logf_row = logf_row + to_row(logf, TOTAL + SEQS * h)
        score_row = score_row + to_row(score_new[h], TOTAL + SEQS * h)
    peaks = tails + shift[...] + logf_row
    peak = jnp.maximum(jnp.max(peaks, axis=0, keepdims=True), score_row)
    lane = iota((N_KV, LANES), 1)
    stats = (lane >= TOTAL) & (lane < TOTAL + 2 * SEQS)
    factors = jnp.where(stats, jnp.exp(jnp.where(stats, peaks - peak, F32(0.0))), F32(0.0))
    weight_new = jnp.exp(jnp.where(stats[0:1], score_row - peak, F32(0.0)))
    den = jnp.sum(factors * pltpu.roll(tails, TOTAL, 1), axis=0, keepdims=True) + weight_new
    width = N_KV * ROWS
    slot, inside = row_of_slot(width)
    expand = (jnp.broadcast_to(slot, (N_KV, width)) == iota((N_KV, width), 0)).astype(F32)
    turned = jnp.transpose(factors)[TOTAL : TOTAL + 2 * SEQS]
    wide = jnp.dot(turned, expand, precision=HI, preferred_element_type=F32)
    own = jnp.broadcast_to(inside, (2 * SEQS, width)) == (iota((2 * SEQS, width), 0) & 7)
    wide = jnp.where(own, wide, F32(0.0))
    both = jnp.dot(wide, slots[...], precision=HI, preferred_element_type=F32)
    low = first_head()
    weighted = jnp.where(low, both[:SEQS], both[SEQS:])

    def lanes_of(row):
        return jnp.where(low, to_column(row, TOTAL), to_column(row, TOTAL + SEQS))

    attended = (weighted + lanes_of(weight_new) * value) / lanes_of(den)
    silu = gate / (1.0 + jnp.exp(-gate))
    gated = (head_norm(attended) * silu).astype(jnp.bfloat16)
    mixed = jnp.zeros((SEQS, w_out.shape[1]), F32)
    for h in range(2):
        half = gated[:, HEAD_DIM * h : HEAD_DIM * (h + 1)]
        mixed = mixed + lax.dot_general(half, w_out[h], NT, preferred_element_type=F32)
    partial_out[...] = mixed


def exchange(slots):
    slots = lax.all_to_all(slots.reshape(N_KV, 1, ROWS * LANES), KV, 0, 0, tiled=True)
    return slots.reshape(N_KV * ROWS, LANES)


def call(kernel, name, *outs):
    shapes = [jax.ShapeDtypeStruct(shape, dtype) for shape, dtype in outs]
    params = pltpu.CompilerParams(vmem_limit_bytes=VMEM)
    return pl.pallas_call(kernel, out_shape=shapes, name=name, compiler_params=params)


def on_device(
    tokens,
    norm_gain,
    w_query,
    w_key,
    w_value,
    w_gate,
    w_forget,
    w_out,
    cache_key,
    cache_value,
    cache_logf,
    lengths,
):
    model = tokens.shape[1]
    limits = (lengths - lax.axis_index(KV) * SPAN)[:, None]
    flat = [w.reshape(model, LANES) for w in (w_query, w_key, w_value, w_gate)]
    logf = jnp.transpose(cache_logf, (2, 0, 1))
    whole = (N_KV * ROWS, LANES)
    tile = (SEQS, LANES)
    (first,) = call(prep, "prep", (whole, F32))(
        tokens, norm_gain[None, :], *flat, jnp.transpose(w_forget), logf, limits
    )
    first = exchange(first)
    second, query, sums, shift = call(
        attend, "attend", (whole, F32), (tile, F32), (tile, F32), ((N_KV, LANES), F32)
    )(
        first,
        jnp.transpose(cache_key, (0, 2, 3, 1)),
        jnp.transpose(cache_value, (0, 2, 3, 1)),
        logf,
        limits,
    )
    second = exchange(second)
    partial_out, key_new, value_new, logf_new = call(
        combine,
        "combine",
        ((SEQS, model), F32),
        (tile, jnp.bfloat16),
        (tile, F32),
        ((2,) + tile, F32),
    )(second, query, sums, shift, jnp.transpose(w_out, (0, 2, 1)))
    mixed = lax.all_gather(partial_out, "tp").sum(0)
    heads = (SEQS, 2, HEAD_DIM)
    return (
        mixed,
        key_new.reshape(heads),
        value_new.reshape(heads),
        jnp.transpose(logf_new[:, :, 0]),
    )


def solution(mesh):
    finer = Mesh(
        mesh.devices.reshape(mesh.shape["dp"], 8, 8, mesh.shape["tp"]), ("dp", "kv_0", "kv_1", "tp")
    )
    return jax.shard_map(
        on_device,
        mesh=finer,
        in_specs=(
            P("dp", KV),
            P(KV),
            P(KV, "tp", None),
            P(KV, "tp", None),
            P(KV, "tp", None),
            P(KV, "tp", None),
            P(KV, "tp"),
            P("tp", None, KV),
            P("dp", KV, "tp", None),
            P("dp", KV, "tp", None),
            P("dp", KV, "tp"),
            P("dp"),
        ),
        out_specs=(P("dp", KV), P("dp", "tp", None), P("dp", "tp", None), P("dp", "tp")),
        check_vma=False,
    )
```

```python
import jax
import jax.numpy as jnp
from jax import lax
from jax.experimental import pallas as pl
from jax.experimental.pallas import tpu as pltpu
from jax.sharding import Mesh
from jax.sharding import PartitionSpec as P

D = 1024
HEAD_DIM = 64
KV = ("kv_0", "kv_1")
N_KV = 64
SEQS = 8
ROWS = 9
VMEM = 16 * 2**20
SPAN = 512
LANES = 128

eps = 1e-06
very_low = -1e30
HI = lax.Precision.HIGHEST
F32 = jnp.float32
NT = (((1,), (1,)), ((), ()))

FORGET, TOTAL, PIECES, PIECE = 8, 24, 40, 16


def iota(shape, dim):
    return lax.broadcasted_iota(jnp.int32, shape, dim)


def to_row(column, start):
    shape = (SEQS, LANES)
    picked = jnp.where(iota(shape, 1) == iota(shape, 0) + start, column, F32(0.0))
    return jnp.sum(picked, axis=0, keepdims=True)


def to_column(row, start):
    shape = (SEQS, LANES)
    picked = jnp.where(iota(shape, 1) == iota(shape, 0) + start, row, F32(0.0))
    return jnp.sum(picked, axis=1, keepdims=True)


def first_head():
    return iota((SEQS, LANES), 1) < HEAD_DIM


def per_head(values):
    low = jnp.sum(jnp.where(first_head(), values, F32(0.0)), axis=1, keepdims=True)
    high = jnp.sum(jnp.where(first_head(), F32(0.0), values), axis=1, keepdims=True)
    return low, high


def head_norm(values):
    low, high = per_head(values * values)
    return values * lax.rsqrt(jnp.where(first_head(), low, high) * (1.0 / HEAD_DIM) + eps)


def between(start, width):
    lane = iota((SEQS, LANES), 1)
    return (lane >= start) & (lane < start + width)


def row_of_slot(width):
    i = iota((1, width), 1)
    slot = (i * 7282) >> 16
    return slot, i - ROWS * slot


def prep(*refs):
    sources, (slots, bias_out, keys, values, w_out, *local, sems) = refs[:12], refs[12:]
    targets = (*local, keys, values, w_out)
    copies = [
        pltpu.make_async_copy(source, target, sems.at[n])
        for n, (source, target) in enumerate(zip(sources, targets))
    ]
    for copy in copies:
        copy.start()
    for copy in copies[:9]:
        copy.wait()
    tokens, gain, w_query, w_key, w_value, w_gate, w_forget, logf, lengths = local
    wide = tokens[...].astype(F32)
    squares = jnp.sum(wide * wide, axis=1, keepdims=True)
    scaled = wide * gain[...]

    def project(weight):
        weight = weight[...].astype(F32)
        halves = [
            jnp.dot(scaled, weight[:, h, :], precision=HI, preferred_element_type=F32)
            for h in range(2)
        ]
        return jnp.concatenate(halves, axis=1)

    forget = lax.dot_general(
        scaled, w_forget[...].astype(F32), NT, precision=HI, preferred_element_type=F32
    )
    shard = lax.axis_index("kv_0") * 8 + lax.axis_index("kv_1")
    limits = jnp.where(iota((SEQS, SEQS), 0) == iota((SEQS, SEQS), 1), lengths[...], 0)
    limits = jnp.sum(limits, axis=1, keepdims=True) - shard * SPAN
    live = iota((SEQS, SPAN), 1) < limits
    shape = (LANES, LANES)
    upper = (iota(shape, 0) > iota(shape, 1)).astype(F32)
    row = to_row(squares, 0)
    for h in range(2):
        gates = jnp.where(live, logf[:, h, :], F32(0.0))
        biases, after = [], jnp.zeros((SEQS, 1), F32)
        for b in reversed(range(SPAN // LANES)):
            part = gates[:, LANES * b : LANES * (b + 1)]
            biases.append(jnp.dot(part, upper, precision=HI, preferred_element_type=F32) + after)
            after = after + jnp.sum(part, axis=1, keepdims=True)
        bias = jnp.concatenate(biases[::-1], axis=1)
        bias_out[pl.ds(SEQS * h, SEQS), :] = jnp.where(live, bias, F32(very_low))
        row = row + to_row(forget[:, h : h + 1], FORGET + SEQS * h)
        row = row + to_row(after, TOTAL + SEQS * h)
    query = project(w_query)
    parts = [project(w) for w in (w_key, w_value, w_gate)]
    for j in range(N_KV):
        slots[pl.ds(ROWS * j, SEQS), :] = query
    for c in range(8):
        tail = jnp.broadcast_to(row, (SEQS, LANES))
        for n, part in enumerate(parts):
            start = PIECES + PIECE * n
            moved = pltpu.roll(part, (start - PIECE * c) % LANES, 1)
            tail = jnp.where(between(start, PIECE), moved, tail)
        slots[pl.ds(ROWS * c + SEQS, SEQS, stride=ROWS * 8), :] = tail
    for copy in copies[9:]:
        copy.wait()


def attend(
    slots, cache_key, cache_value, bias, send, query_out, sums_out, shift_out, logf_out
):
    got = slots[...]
    width = N_KV * ROWS
    _, inside = row_of_slot(width)
    picks = (jnp.broadcast_to(inside, (16, width)) == iota((16, width), 0)).astype(F32)
    summed = jnp.dot(picks, got, precision=HI, preferred_element_type=F32)
    raw = summed[:SEQS]
    sums = summed[SEQS : SEQS + 1]
    inv_root = lax.rsqrt(to_column(sums, 0) * (1.0 / D) + eps)
    query = head_norm(raw * inv_root).astype(jnp.bfloat16)
    query_out[...] = query.astype(F32)
    sums_out[...] = jnp.broadcast_to(sums, (SEQS, LANES))

    logf_row = jnp.zeros((1, LANES), F32)
    for h in range(2):
        forget = to_column(sums, FORGET + SEQS * h) * inv_root
        logf = jnp.minimum(forget, 0.0) - jnp.log1p(jnp.exp(-jnp.abs(forget)))
        logf_out[pl.ds(h, 1), :] = to_row(logf, 0)[:, :SEQS]
        logf_row = logf_row + to_row(logf, TOTAL + SEQS * h)
    tails = slots[pl.ds(SEQS, N_KV, stride=ROWS), :]
    shape = (N_KV, N_KV)
    upper = (iota(shape, 1) > iota(shape, 0)).astype(F32)
    later = jnp.dot(upper, tails, precision=HI, preferred_element_type=F32)
    shift_out[...] = later + logf_row

    blocks = []
    wide_query = query.astype(F32)
    seq = iota((SEQS, LANES), 0)
    for s in range(SEQS):
        mine = jnp.where(seq == s, wide_query, F32(0.0))
        low = jnp.where(first_head(), mine, F32(0.0))
        blocks.append(jnp.concatenate([low, mine - low], axis=0))
    spread = jnp.concatenate(blocks, axis=1).astype(jnp.bfloat16)
    keys = cache_key[...].reshape(SEQS * LANES, SPAN)
    scores = jnp.dot(spread, keys, preferred_element_type=F32) * HEAD_DIM ** (-0.5)

    live = bias[...] > F32(0.5 * very_low)
    scores = jnp.where(live, scores + bias[...], F32(very_low))
    peak = jnp.max(scores, axis=1, keepdims=True)
    weights = jnp.where(live, jnp.exp(scores - peak), F32(0.0))
    den = jnp.sum(weights, axis=1, keepdims=True)
    values = cache_value[...].reshape(SEQS * LANES, SPAN)
    crossed = lax.dot_general(
        weights.astype(jnp.bfloat16), values, NT, preferred_element_type=F32
    )
    local = jnp.zeros((SEQS, LANES), F32)
    for s in range(SEQS):
        block = crossed[:, LANES * s : LANES * (s + 1)]
        own = jnp.where(first_head(), block[:SEQS], block[SEQS:])
        local = jnp.where(seq == s, own, local)
    lane = iota((1, LANES), 1)
    row = jnp.where((lane >= PIECES) & (lane < PIECES + 3 * PIECE), sums, F32(0.0))
    for h in range(2):
        rows = slice(SEQS * h, SEQS * (h + 1))
        row = row + to_row(den[rows], SEQS * h) + to_row(peak[rows], TOTAL + SEQS * h)
    tail = jnp.broadcast_to(row, (SEQS, LANES))
    for j in range(N_KV):
        send[pl.ds(ROWS * j, SEQS), :] = local
    for c in range(8):
        send[pl.ds(ROWS * c + SEQS, SEQS, stride=ROWS * 8), :] = tail


def combine(slots, query, sums, shift, w_out, partial_out, key_out, value_out):
    sums_row = sums[0:1, :]
    inv_root = lax.rsqrt(to_column(sums_row, 0) * (1.0 / D) + eps)
    parts = [jnp.zeros((SEQS, LANES), F32) for _ in range(3)]
    for c in range(8):
        tail = slots[pl.ds(ROWS * c + SEQS, SEQS, stride=ROWS * 8), :]
        for n in range(3):
            start = PIECES + PIECE * n
            moved = pltpu.roll(tail, (PIECE * c - start) % LANES, 1)
            parts[n] = jnp.where(between(PIECE * c, PIECE), moved, parts[n])
    key, value, gate = (part * inv_root for part in parts)
    key = head_norm(key).astype(jnp.bfloat16)
    for h in range(2):
        part = slice(HEAD_DIM * h, HEAD_DIM * (h + 1))
        key_out[:, h, :] = key[:, part]
        value_out[:, h, :] = value[:, part]
    score_new = [x * HEAD_DIM ** (-0.5) for x in per_head(query[...] * key.astype(F32))]
    tails = slots[pl.ds(SEQS, N_KV, stride=ROWS), :]
    score_row = jnp.zeros((1, LANES), F32)
    for h in range(2):
        score_row = score_row + to_row(score_new[h], TOTAL + SEQS * h)
    peaks = tails + shift[...]
    peak = jnp.maximum(jnp.max(peaks, axis=0, keepdims=True), score_row)
    lane = iota((N_KV, LANES), 1)
    stats = (lane >= TOTAL) & (lane < TOTAL + 2 * SEQS)
    factors = jnp.where(stats, jnp.exp(jnp.where(stats, peaks - peak, F32(0.0))), F32(0.0))
    weight_new = jnp.exp(jnp.where(stats[0:1], score_row - peak, F32(0.0)))
    den = jnp.sum(factors * pltpu.roll(tails, TOTAL, 1), axis=0, keepdims=True) + weight_new
    width = N_KV * ROWS
    slot, inside = row_of_slot(width)
    expand = (jnp.broadcast_to(slot, (N_KV, width)) == iota((N_KV, width), 0)).astype(F32)
    turned = jnp.transpose(factors)[TOTAL : TOTAL + 2 * SEQS]
    wide = jnp.dot(turned, expand, precision=HI, preferred_element_type=F32)
    own = jnp.broadcast_to(inside, (2 * SEQS, width)) == (iota((2 * SEQS, width), 0) & 7)
    wide = jnp.where(own, wide, F32(0.0))
    both = jnp.dot(wide, slots[...], precision=HI, preferred_element_type=F32)
    low = first_head()
    weighted = jnp.where(low, both[:SEQS], both[SEQS:])

    def lanes_of(row):
        return jnp.where(low, to_column(row, TOTAL), to_column(row, TOTAL + SEQS))

    attended = (weighted + lanes_of(weight_new) * value) / lanes_of(den)
    silu = gate / (1.0 + jnp.exp(-gate))
    gated = (head_norm(attended) * silu).astype(jnp.bfloat16)
    mixed = jnp.zeros((SEQS, w_out.shape[1]), F32)
    for h in range(2):
        half = gated[:, HEAD_DIM * h : HEAD_DIM * (h + 1)]
        mixed = mixed + lax.dot_general(half, w_out[h], NT, preferred_element_type=F32)
    partial_out[...] = mixed


def exchange(slots):
    slots = lax.all_to_all(slots.reshape(N_KV, 1, ROWS * LANES), KV, 0, 0, tiled=True)
    return slots.reshape(N_KV * ROWS, LANES)


def call(kernel, name, outs, operands, **more):
    shapes = [jax.ShapeDtypeStruct(shape, dtype) for shape, dtype in outs]
    params = pltpu.CompilerParams(vmem_limit_bytes=VMEM)
    run = pl.pallas_call(kernel, out_shape=shapes, name=name, compiler_params=params, **more)
    return run(*operands)


def on_device(
    tokens,
    norm_gain,
    w_query,
    w_key,
    w_value,
    w_gate,
    w_forget,
    w_out,
    cache_key,
    cache_value,
    cache_logf,
    lengths,
):
    whole = ((N_KV * ROWS, LANES), F32)
    tile = ((SEQS, LANES), F32)
    small = (tokens, norm_gain[None, :], w_query, w_key, w_value, w_gate, jnp.transpose(w_forget))
    small = small + (jnp.transpose(cache_logf, (0, 2, 1)), lengths[None, :])
    large = [jnp.transpose(cache, (0, 2, 3, 1)) for cache in (cache_key, cache_value)]
    large.append(jnp.transpose(w_out, (0, 2, 1)))
    first, bias, keys, values, w_out = call(
        prep,
        "prep",
        [whole, ((2 * SEQS, SPAN), F32)] + [(x.shape, x.dtype) for x in large],
        [pltpu.with_memory_space_constraint(x, pltpu.HBM) for x in (*small, *large)],
        in_specs=[pl.BlockSpec(memory_space=pltpu.HBM)] * 12,
        scratch_shapes=[pltpu.VMEM(x.shape, x.dtype) for x in small]
        + [pltpu.SemaphoreType.DMA((12,))],
    )
    second, query, sums, shift, logf_new = call(
        attend,
        "attend",
        [whole, tile, tile, ((N_KV, LANES), F32), ((2, SEQS), F32)],
        (exchange(first), keys, values, bias),
    )
    heads = (SEQS, 2, HEAD_DIM)
    partial_out, key_new, value_new = call(
        combine,
        "combine",
        [((SEQS, tokens.shape[1]), F32), (heads, jnp.bfloat16), (heads, F32)],
        (exchange(second), query, sums, shift, w_out),
    )
    mixed = lax.all_gather(partial_out, "tp").sum(0)
    return mixed, key_new, value_new, jnp.transpose(logf_new)


def solution(mesh):
    finer = Mesh(
        mesh.devices.reshape(mesh.shape["dp"], 8, 8, mesh.shape["tp"]), ("dp", "kv_0", "kv_1", "tp")
    )
    return jax.shard_map(
        on_device,
        mesh=finer,
        in_specs=(
            P("dp", KV),
            P(KV),
            P(KV, "tp", None),
            P(KV, "tp", None),
            P(KV, "tp", None),
            P(KV, "tp", None),
            P(KV, "tp"),
            P("tp", None, KV),
            P("dp", KV, "tp", None),
            P("dp", KV, "tp", None),
            P("dp", KV, "tp"),
            P("dp"),
        ),
        out_specs=(P("dp", KV), P("dp", "tp", None), P("dp", "tp", None), P("dp", "tp")),
        check_vma=False,
    )
```

```python
import jax
import jax.numpy as jnp
from jax import lax
from jax.experimental import pallas as pl
from jax.experimental.pallas import tpu as pltpu
from jax.sharding import Mesh
from jax.sharding import PartitionSpec as P

D = 1024
HEAD_DIM = 64
KV = ("kv_0", "kv_1")
N_KV = 64
SEQS = 8
ROWS = 9
VMEM = 16 * 2**20
SPAN = 512
LANES = 128

eps = 1e-06
very_low = -1e30
HI = lax.Precision.HIGHEST
F32 = jnp.float32
NT = (((1,), (1,)), ((), ()))

FORGET, TOTAL, PIECES, PIECE = 8, 24, 40, 16


def iota(shape, dim):
    return lax.broadcasted_iota(jnp.int32, shape, dim)


def to_row(column, start):
    shape = (SEQS, LANES)
    picked = jnp.where(iota(shape, 1) == iota(shape, 0) + start, column, F32(0.0))
    return jnp.sum(picked, axis=0, keepdims=True)


def to_column(row, start):
    shape = (SEQS, LANES)
    picked = jnp.where(iota(shape, 1) == iota(shape, 0) + start, row, F32(0.0))
    return jnp.sum(picked, axis=1, keepdims=True)


def first_head():
    return iota((SEQS, LANES), 1) < HEAD_DIM


def per_head(values):
    low = jnp.sum(jnp.where(first_head(), values, F32(0.0)), axis=1, keepdims=True)
    high = jnp.sum(jnp.where(first_head(), F32(0.0), values), axis=1, keepdims=True)
    return low, high


def head_norm(values):
    low, high = per_head(values * values)
    return values * lax.rsqrt(jnp.where(first_head(), low, high) * (1.0 / HEAD_DIM) + eps)


def between(start, width):
    lane = iota((SEQS, LANES), 1)
    return (lane >= start) & (lane < start + width)


def rows_at(start):
    return pl.ds(start, SEQS, stride=ROWS)


def fill(slots, values):
    for s in range(SEQS):
        row = jnp.broadcast_to(values[s : s + 1, :], (SEQS, LANES))
        for g in range(N_KV // SEQS):
            slots[rows_at(ROWS * SEQS * g + s), :] = row


def total_row(slots, r):
    parts = [slots[rows_at(ROWS * SEQS * g + r), :] for g in range(N_KV // SEQS)]
    while len(parts) > 1:
        parts = [a + b for a, b in zip(parts[::2], parts[1::2])]
    return jnp.sum(parts[0], axis=0, keepdims=True)


def prep(*refs):
    sources, (slots, bias_out, keys, values, w_out, *local, sems) = refs[:12], refs[12:]
    targets = (*local, keys, values, w_out)
    copies = [
        pltpu.make_async_copy(source, target, sems.at[n])
        for n, (source, target) in enumerate(zip(sources, targets))
    ]
    for copy in copies:
        copy.start()
    for copy in copies[:9]:
        copy.wait()
    tokens, gain, w_query, w_key, w_value, w_gate, w_forget, logf, lengths = local
    wide = tokens[...].astype(F32)
    squares = jnp.sum(wide * wide, axis=1, keepdims=True)
    scaled = wide * gain[...]

    def project(weight):
        weight = weight[...].astype(F32)
        halves = [
            jnp.dot(scaled, weight[:, h, :], precision=HI, preferred_element_type=F32)
            for h in range(2)
        ]
        return jnp.concatenate(halves, axis=1)

    forget = lax.dot_general(
        scaled, w_forget[...].astype(F32), NT, precision=HI, preferred_element_type=F32
    )
    shard = lax.axis_index("kv_0") * 8 + lax.axis_index("kv_1")
    limits = jnp.where(iota((SEQS, SEQS), 0) == iota((SEQS, SEQS), 1), lengths[...], 0)
    limits = jnp.sum(limits, axis=1, keepdims=True) - shard * SPAN
    live = iota((SEQS, SPAN), 1) < limits
    shape = (LANES, LANES)
    upper = (iota(shape, 0) > iota(shape, 1)).astype(F32)
    row = to_row(squares, 0)
    for h in range(2):
        gates = jnp.where(live, logf[:, h, :], F32(0.0))
        biases, after = [], jnp.zeros((SEQS, 1), F32)
        for b in reversed(range(SPAN // LANES)):
            part = gates[:, LANES * b : LANES * (b + 1)]
            biases.append(jnp.dot(part, upper, precision=HI, preferred_element_type=F32) + after)
            after = after + jnp.sum(part, axis=1, keepdims=True)
        bias = jnp.concatenate(biases[::-1], axis=1)
        bias_out[pl.ds(SEQS * h, SEQS), :] = jnp.where(live, bias, F32(very_low))
        row = row + to_row(forget[:, h : h + 1], FORGET + SEQS * h)
        row = row + to_row(after, TOTAL + SEQS * h)
    query = project(w_query)
    parts = [project(w) for w in (w_key, w_value, w_gate)]
    fill(slots, query)
    for c in range(8):
        tail = jnp.broadcast_to(row, (SEQS, LANES))
        for n, part in enumerate(parts):
            start = PIECES + PIECE * n
            moved = pltpu.roll(part, (start - PIECE * c) % LANES, 1)
            tail = jnp.where(between(start, PIECE), moved, tail)
        slots[pl.ds(ROWS * c + SEQS, SEQS, stride=ROWS * 8), :] = tail
    for copy in copies[9:]:
        copy.wait()


def attend(
    slots, cache_key, cache_value, bias, send, query_out, sums_out, shift_out, logf_out
):
    seq = iota((SEQS, LANES), 0)
    raw = jnp.zeros((SEQS, LANES), F32)
    for s in range(SEQS):
        raw = jnp.where(seq == s, total_row(slots, s), raw)
    sums = total_row(slots, SEQS)
    inv_root = lax.rsqrt(to_column(sums, 0) * (1.0 / D) + eps)
    query = head_norm(raw * inv_root).astype(jnp.bfloat16)
    query_out[...] = query.astype(F32)
    sums_out[...] = jnp.broadcast_to(sums, (SEQS, LANES))

    logf_row = jnp.zeros((1, LANES), F32)
    for h in range(2):
        forget = to_column(sums, FORGET + SEQS * h) * inv_root
        logf = jnp.minimum(forget, 0.0) - jnp.log1p(jnp.exp(-jnp.abs(forget)))
        logf_out[pl.ds(h, 1), :] = to_row(logf, 0)[:, :SEQS]
        logf_row = logf_row + to_row(logf, TOTAL + SEQS * h)
    tails = slots[pl.ds(SEQS, N_KV, stride=ROWS), :]
    shape = (N_KV, N_KV)
    upper = (iota(shape, 1) > iota(shape, 0)).astype(F32)
    later = jnp.dot(upper, tails, precision=HI, preferred_element_type=F32)
    shift_out[...] = later + logf_row

    blocks = []
    wide_query = query.astype(F32)
    for s in range(SEQS):
        mine = jnp.where(seq == s, wide_query, F32(0.0))
        low = jnp.where(first_head(), mine, F32(0.0))
        blocks.append(jnp.concatenate([low, mine - low], axis=0))
    spread = jnp.concatenate(blocks, axis=1).astype(jnp.bfloat16)
    keys = cache_key[...].reshape(SEQS * LANES, SPAN)
    scores = jnp.dot(spread, keys, preferred_element_type=F32) * HEAD_DIM ** (-0.5)

    live = bias[...] > F32(0.5 * very_low)
    scores = jnp.where(live, scores + bias[...], F32(very_low))
    peak = jnp.max(scores, axis=1, keepdims=True)
    weights = jnp.where(live, jnp.exp(scores - peak), F32(0.0))
    den = jnp.sum(weights, axis=1, keepdims=True)
    values = cache_value[...].reshape(SEQS * LANES, SPAN)
    crossed = lax.dot_general(
        weights.astype(jnp.bfloat16), values, NT, preferred_element_type=F32
    )
    local = jnp.zeros((SEQS, LANES), F32)
    for s in range(SEQS):
        block = crossed[:, LANES * s : LANES * (s + 1)]
        own = jnp.where(first_head(), block[:SEQS], block[SEQS:])
        local = jnp.where(seq == s, own, local)
    lane = iota((1, LANES), 1)
    row = jnp.where((lane >= PIECES) & (lane < PIECES + 3 * PIECE), sums, F32(0.0))
    for h in range(2):
        rows = slice(SEQS * h, SEQS * (h + 1))
        row = row + to_row(den[rows], SEQS * h) + to_row(peak[rows], TOTAL + SEQS * h)
    tail = jnp.broadcast_to(row, (SEQS, LANES))
    fill(send, local)
    for c in range(8):
        send[pl.ds(ROWS * c + SEQS, SEQS, stride=ROWS * 8), :] = tail


def combine(slots, query, sums, shift, w_out, partial_out, key_out, value_out):
    sums_row = sums[0:1, :]
    inv_root = lax.rsqrt(to_column(sums_row, 0) * (1.0 / D) + eps)
    parts = [jnp.zeros((SEQS, LANES), F32) for _ in range(3)]
    for c in range(8):
        tail = slots[pl.ds(ROWS * c + SEQS, SEQS, stride=ROWS * 8), :]
        for n in range(3):
            start = PIECES + PIECE * n
            moved = pltpu.roll(tail, (PIECE * c - start) % LANES, 1)
            parts[n] = jnp.where(between(PIECE * c, PIECE), moved, parts[n])
    key, value, gate = (part * inv_root for part in parts)
    key = head_norm(key).astype(jnp.bfloat16)
    for h in range(2):
        part = slice(HEAD_DIM * h, HEAD_DIM * (h + 1))
        key_out[:, h, :] = key[:, part]
        value_out[:, h, :] = value[:, part]
    score_new = [x * HEAD_DIM ** (-0.5) for x in per_head(query[...] * key.astype(F32))]
    tails = slots[pl.ds(SEQS, N_KV, stride=ROWS), :]
    score_row = jnp.zeros((1, LANES), F32)
    for h in range(2):
        score_row = score_row + to_row(score_new[h], TOTAL + SEQS * h)
    peaks = tails + shift[...]
    peak = jnp.maximum(jnp.max(peaks, axis=0, keepdims=True), score_row)
    lane = iota((N_KV, LANES), 1)
    stats = (lane >= TOTAL) & (lane < TOTAL + 2 * SEQS)
    factors = jnp.where(stats, jnp.exp(jnp.where(stats, peaks - peak, F32(0.0))), F32(0.0))
    weight_new = jnp.exp(jnp.where(stats[0:1], score_row - peak, F32(0.0)))
    den = jnp.sum(factors * pltpu.roll(tails, TOTAL, 1), axis=0, keepdims=True) + weight_new
    low, seq = first_head(), iota((SEQS, LANES), 0)
    weighted = jnp.zeros((SEQS, LANES), F32)
    for s in range(SEQS):
        sums_of = []
        for g in range(N_KV // SEQS):
            own = factors[SEQS * g : SEQS * (g + 1)]
            first, second = (own[:, n : n + 1] for n in (TOTAL + s, TOTAL + SEQS + s))
            sums_of.append(jnp.where(low, first, second) * slots[rows_at(ROWS * SEQS * g + s), :])
        while len(sums_of) > 1:
            sums_of = [a + b for a, b in zip(sums_of[::2], sums_of[1::2])]
        weighted = jnp.where(seq == s, jnp.sum(sums_of[0], axis=0, keepdims=True), weighted)

    def lanes_of(row):
        return jnp.where(low, to_column(row, TOTAL), to_column(row, TOTAL + SEQS))

    attended = (weighted + lanes_of(weight_new) * value) / lanes_of(den)
    silu = gate / (1.0 + jnp.exp(-gate))
    gated = (head_norm(attended) * silu).astype(jnp.bfloat16)
    mixed = jnp.zeros((SEQS, w_out.shape[1]), F32)
    for h in range(2):
        half = gated[:, HEAD_DIM * h : HEAD_DIM * (h + 1)]
        mixed = mixed + lax.dot_general(half, w_out[h], NT, preferred_element_type=F32)
    partial_out[...] = mixed


def exchange(slots):
    slots = lax.all_to_all(slots.reshape(N_KV, 1, ROWS * LANES), KV, 0, 0, tiled=True)
    return slots.reshape(N_KV * ROWS, LANES)


def call(kernel, name, outs, operands, **more):
    shapes = [jax.ShapeDtypeStruct(shape, dtype) for shape, dtype in outs]
    params = pltpu.CompilerParams(vmem_limit_bytes=VMEM)
    run = pl.pallas_call(kernel, out_shape=shapes, name=name, compiler_params=params, **more)
    return run(*operands)


def on_device(
    tokens,
    norm_gain,
    w_query,
    w_key,
    w_value,
    w_gate,
    w_forget,
    w_out,
    cache_key,
    cache_value,
    cache_logf,
    lengths,
):
    whole = ((N_KV * ROWS, LANES), F32)
    tile = ((SEQS, LANES), F32)
    small = (tokens, norm_gain[None, :], w_query, w_key, w_value, w_gate, jnp.transpose(w_forget))
    small = small + (jnp.transpose(cache_logf, (0, 2, 1)), lengths[None, :])
    large = [jnp.transpose(cache, (0, 2, 3, 1)) for cache in (cache_key, cache_value)]
    large.append(jnp.transpose(w_out, (0, 2, 1)))
    first, bias, keys, values, w_out = call(
        prep,
        "prep",
        [whole, ((2 * SEQS, SPAN), F32)] + [(x.shape, x.dtype) for x in large],
        [pltpu.with_memory_space_constraint(x, pltpu.HBM) for x in (*small, *large)],
        in_specs=[pl.BlockSpec(memory_space=pltpu.HBM)] * 12,
        scratch_shapes=[pltpu.VMEM(x.shape, x.dtype) for x in small]
        + [pltpu.SemaphoreType.DMA((12,))],
    )
    second, query, sums, shift, logf_new = call(
        attend,
        "attend",
        [whole, tile, tile, ((N_KV, LANES), F32), ((2, SEQS), F32)],
        (exchange(first), keys, values, bias),
    )
    heads = (SEQS, 2, HEAD_DIM)
    partial_out, key_new, value_new = call(
        combine,
        "combine",
        [((SEQS, tokens.shape[1]), F32), (heads, jnp.bfloat16), (heads, F32)],
        (exchange(second), query, sums, shift, w_out),
    )
    mixed = lax.all_gather(partial_out, "tp").sum(0)
    return mixed, key_new, value_new, jnp.transpose(logf_new)


def solution(mesh):
    finer = Mesh(
        mesh.devices.reshape(mesh.shape["dp"], 8, 8, mesh.shape["tp"]), ("dp", "kv_0", "kv_1", "tp")
    )
    return jax.shard_map(
        on_device,
        mesh=finer,
        in_specs=(
            P("dp", KV),
            P(KV),
            P(KV, "tp", None),
            P(KV, "tp", None),
            P(KV, "tp", None),
            P(KV, "tp", None),
            P(KV, "tp"),
            P("tp", None, KV),
            P("dp", KV, "tp", None),
            P("dp", KV, "tp", None),
            P("dp", KV, "tp"),
            P("dp"),
        ),
        out_specs=(P("dp", KV), P("dp", "tp", None), P("dp", "tp", None), P("dp", "tp")),
        check_vma=False,
    )
```

```python
import jax
import jax.numpy as jnp
from jax import lax
from jax.experimental import pallas as pl
from jax.experimental.pallas import tpu as pltpu
from jax.sharding import Mesh
from jax.sharding import PartitionSpec as P

D = 1024
HEAD_DIM = 64
KV = ("kv_0", "kv_1")
N_KV = 64
SEQS = 8
ROWS = 9
VMEM = 16 * 2**20
SPAN = 512
LANES = 128

eps = 1e-06
very_low = -1e30
HI = lax.Precision.HIGHEST
F32 = jnp.float32
NT = (((1,), (1,)), ((), ()))

FORGET, TOTAL, PIECES, PIECE = 8, 24, 40, 16


def iota(shape, dim):
    return lax.broadcasted_iota(jnp.int32, shape, dim)


def to_row(column, start):
    shape = (SEQS, LANES)
    picked = jnp.where(iota(shape, 1) == iota(shape, 0) + start, column, F32(0.0))
    return jnp.sum(picked, axis=0, keepdims=True)


def to_column(row, start):
    shape = (SEQS, LANES)
    picked = jnp.where(iota(shape, 1) == iota(shape, 0) + start, row, F32(0.0))
    return jnp.sum(picked, axis=1, keepdims=True)


def first_head():
    return iota((SEQS, LANES), 1) < HEAD_DIM


def per_head(values):
    low = jnp.sum(jnp.where(first_head(), values, F32(0.0)), axis=1, keepdims=True)
    high = jnp.sum(jnp.where(first_head(), F32(0.0), values), axis=1, keepdims=True)
    return low, high


def head_norm(values):
    low, high = per_head(values * values)
    return values * lax.rsqrt(jnp.where(first_head(), low, high) * (1.0 / HEAD_DIM) + eps)


def between(start, width):
    lane = iota((SEQS, LANES), 1)
    return (lane >= start) & (lane < start + width)


def rows_at(start):
    return pl.ds(start, SEQS, stride=ROWS)


def fill(slots, values):
    for s in range(SEQS):
        row = jnp.broadcast_to(values[s : s + 1, :], (SEQS, LANES))
        for g in range(N_KV // SEQS):
            slots[rows_at(ROWS * SEQS * g + s), :] = row


def total_row(slots, r):
    parts = [slots[rows_at(ROWS * SEQS * g + r), :] for g in range(N_KV // SEQS)]
    while len(parts) > 1:
        parts = [a + b for a, b in zip(parts[::2], parts[1::2])]
    return jnp.sum(parts[0], axis=0, keepdims=True)


def prep(*refs):
    sources, (slots, bias_out, keys, values, w_out, *local, sems) = refs[:12], refs[12:]
    targets = (*local, keys, values, w_out)
    copies = [
        pltpu.make_async_copy(source, target, sems.at[n])
        for n, (source, target) in enumerate(zip(sources, targets))
    ]
    for copy in copies:
        copy.start()
    for copy in copies[:9]:
        copy.wait()
    tokens, gain, w_query, w_key, w_value, w_gate, w_forget, logf, lengths = local
    wide = tokens[...].astype(F32)
    squares = jnp.sum(wide * wide, axis=1, keepdims=True)
    scaled = wide * gain[...]

    wide_weights = [w[...].astype(F32) for w in (w_query, w_key, w_value, w_gate)]
    halves = [w[:, h, :] for w in wide_weights for h in range(2)]
    products = jnp.dot(
        scaled, jnp.concatenate(halves, axis=1), precision=HI, preferred_element_type=F32
    )
    forget = lax.dot_general(
        scaled, w_forget[...].astype(F32), NT, precision=HI, preferred_element_type=F32
    )
    shard = lax.axis_index("kv_0") * 8 + lax.axis_index("kv_1")
    limits = jnp.where(iota((SEQS, SEQS), 0) == iota((SEQS, SEQS), 1), lengths[...], 0)
    limits = jnp.sum(limits, axis=1, keepdims=True) - shard * SPAN
    live = iota((SEQS, SPAN), 1) < limits
    shape = (LANES, LANES)
    upper = (iota(shape, 0) > iota(shape, 1)).astype(F32)
    row = to_row(squares, 0)
    blocks = SPAN // LANES
    gates = []
    for h in range(2):
        masked = jnp.where(live, logf[:, h, :], F32(0.0))
        gates += [masked[:, LANES * b : LANES * (b + 1)] for b in range(blocks)]
    inside = jnp.dot(
        jnp.concatenate(gates, axis=0), upper, precision=HI, preferred_element_type=F32
    )
    for h in range(2):
        biases, after = [], jnp.zeros((SEQS, 1), F32)
        for n in reversed(range(blocks * h, blocks * (h + 1))):
            biases.append(inside[SEQS * n : SEQS * (n + 1)] + after)
            after = after + jnp.sum(gates[n], axis=1, keepdims=True)
        bias = jnp.concatenate(biases[::-1], axis=1)
        bias_out[pl.ds(SEQS * h, SEQS), :] = jnp.where(live, bias, F32(very_low))
        row = row + to_row(forget[:, h : h + 1], FORGET + SEQS * h)
        row = row + to_row(after, TOTAL + SEQS * h)
    query, *parts = [products[:, LANES * n : LANES * (n + 1)] for n in range(4)]
    fill(slots, query)
    for c in range(8):
        tail = jnp.broadcast_to(row, (SEQS, LANES))
        for n, part in enumerate(parts):
            start = PIECES + PIECE * n
            moved = pltpu.roll(part, (start - PIECE * c) % LANES, 1)
            tail = jnp.where(between(start, PIECE), moved, tail)
        slots[pl.ds(ROWS * c + SEQS, SEQS, stride=ROWS * 8), :] = tail
    for copy in copies[9:]:
        copy.wait()


def attend(
    slots, cache_key, cache_value, bias, send, query_out, sums_out, shift_out, logf_out, logf_here, sem
):
    seq = iota((SEQS, LANES), 0)
    raw = jnp.zeros((SEQS, LANES), F32)
    for s in range(SEQS):
        raw = jnp.where(seq == s, total_row(slots, s), raw)
    sums = total_row(slots, SEQS)
    inv_root = lax.rsqrt(to_column(sums, 0) * (1.0 / D) + eps)
    query = head_norm(raw * inv_root).astype(jnp.bfloat16)
    query_out[...] = query.astype(F32)
    sums_out[...] = jnp.broadcast_to(sums, (SEQS, LANES))

    logf_row = jnp.zeros((1, LANES), F32)
    for h in range(2):
        forget = to_column(sums, FORGET + SEQS * h) * inv_root
        logf = jnp.minimum(forget, 0.0) - jnp.log1p(jnp.exp(-jnp.abs(forget)))
        logf_here[pl.ds(h, 1), :] = to_row(logf, 0)[:, :SEQS]
        logf_row = logf_row + to_row(logf, TOTAL + SEQS * h)
    copy = pltpu.make_async_copy(logf_here, logf_out, sem)
    copy.start()
    tails = slots[pl.ds(SEQS, N_KV, stride=ROWS), :]
    shape = (N_KV, N_KV)
    upper = (iota(shape, 1) > iota(shape, 0)).astype(F32)
    later = jnp.dot(upper, tails, precision=HI, preferred_element_type=F32)
    shift_out[...] = later + logf_row

    blocks = []
    wide_query = query.astype(F32)
    for s in range(SEQS):
        mine = jnp.where(seq == s, wide_query, F32(0.0))
        low = jnp.where(first_head(), mine, F32(0.0))
        blocks.append(jnp.concatenate([low, mine - low], axis=0))
    spread = jnp.concatenate(blocks, axis=1).astype(jnp.bfloat16)
    keys = cache_key[...].reshape(SEQS * LANES, SPAN)
    scores = jnp.dot(spread, keys, preferred_element_type=F32) * HEAD_DIM ** (-0.5)

    live = bias[...] > F32(0.5 * very_low)
    scores = jnp.where(live, scores + bias[...], F32(very_low))
    peak = jnp.max(scores, axis=1, keepdims=True)
    weights = jnp.where(live, jnp.exp(scores - peak), F32(0.0))
    den = jnp.sum(weights, axis=1, keepdims=True)
    values = cache_value[...].reshape(SEQS * LANES, SPAN)
    crossed = lax.dot_general(
        weights.astype(jnp.bfloat16), values, NT, preferred_element_type=F32
    )
    local = jnp.zeros((SEQS, LANES), F32)
    for s in range(SEQS):
        block = crossed[:, LANES * s : LANES * (s + 1)]
        own = jnp.where(first_head(), block[:SEQS], block[SEQS:])
        local = jnp.where(seq == s, own, local)
    lane = iota((1, LANES), 1)
    row = jnp.where((lane >= PIECES) & (lane < PIECES + 3 * PIECE), sums, F32(0.0))
    for h in range(2):
        rows = slice(SEQS * h, SEQS * (h + 1))
        row = row + to_row(den[rows], SEQS * h) + to_row(peak[rows], TOTAL + SEQS * h)
    tail = jnp.broadcast_to(row, (SEQS, LANES))
    fill(send, local)
    for c in range(8):
        send[pl.ds(ROWS * c + SEQS, SEQS, stride=ROWS * 8), :] = tail
    copy.wait()


def combine(
    slots, query, sums, shift, w_out, partial_out, key_out, value_out, key_here, value_here, sems
):
    sums_row = sums[0:1, :]
    inv_root = lax.rsqrt(to_column(sums_row, 0) * (1.0 / D) + eps)
    parts = [jnp.zeros((SEQS, LANES), F32) for _ in range(3)]
    for c in range(8):
        tail = slots[pl.ds(ROWS * c + SEQS, SEQS, stride=ROWS * 8), :]
        for n in range(3):
            start = PIECES + PIECE * n
            moved = pltpu.roll(tail, (PIECE * c - start) % LANES, 1)
            parts[n] = jnp.where(between(PIECE * c, PIECE), moved, parts[n])
    key, value, gate = (part * inv_root for part in parts)
    key = head_norm(key).astype(jnp.bfloat16)
    for h in range(2):
        part = slice(HEAD_DIM * h, HEAD_DIM * (h + 1))
        key_here[:, h, :] = key[:, part]
        value_here[:, h, :] = value[:, part]
    copies = [
        pltpu.make_async_copy(key_here, key_out, sems.at[0]),
        pltpu.make_async_copy(value_here, value_out, sems.at[1]),
    ]
    for copy in copies:
        copy.start()
    score_new = [x * HEAD_DIM ** (-0.5) for x in per_head(query[...] * key.astype(F32))]
    tails = slots[pl.ds(SEQS, N_KV, stride=ROWS), :]
    score_row = jnp.zeros((1, LANES), F32)
    for h in range(2):
        score_row = score_row + to_row(score_new[h], TOTAL + SEQS * h)
    peaks = tails + shift[...]
    peak = jnp.maximum(jnp.max(peaks, axis=0, keepdims=True), score_row)
    lane = iota((N_KV, LANES), 1)
    stats = (lane >= TOTAL) & (lane < TOTAL + 2 * SEQS)
    factors = jnp.where(stats, jnp.exp(jnp.where(stats, peaks - peak, F32(0.0))), F32(0.0))
    weight_new = jnp.exp(jnp.where(stats[0:1], score_row - peak, F32(0.0)))
    den = jnp.sum(factors * pltpu.roll(tails, TOTAL, 1), axis=0, keepdims=True) + weight_new
    low, seq = first_head(), iota((SEQS, LANES), 0)
    weighted = jnp.zeros((SEQS, LANES), F32)
    for s in range(SEQS):
        sums_of = []
        for g in range(N_KV // SEQS):
            own = factors[SEQS * g : SEQS * (g + 1)]
            first, second = (own[:, n : n + 1] for n in (TOTAL + s, TOTAL + SEQS + s))
            sums_of.append(jnp.where(low, first, second) * slots[rows_at(ROWS * SEQS * g + s), :])
        while len(sums_of) > 1:
            sums_of = [a + b for a, b in zip(sums_of[::2], sums_of[1::2])]
        weighted = jnp.where(seq == s, jnp.sum(sums_of[0], axis=0, keepdims=True), weighted)

    def lanes_of(row):
        return jnp.where(low, to_column(row, TOTAL), to_column(row, TOTAL + SEQS))

    attended = (weighted + lanes_of(weight_new) * value) / lanes_of(den)
    silu = gate / (1.0 + jnp.exp(-gate))
    gated = (head_norm(attended) * silu).astype(jnp.bfloat16)
    mixed = jnp.zeros((SEQS, w_out.shape[1]), F32)
    for h in range(2):
        half = gated[:, HEAD_DIM * h : HEAD_DIM * (h + 1)]
        mixed = mixed + lax.dot_general(half, w_out[h], NT, preferred_element_type=F32)
    partial_out[...] = mixed
    for copy in copies:
        copy.wait()


def exchange(slots):
    slots = lax.all_to_all(slots.reshape(N_KV, 1, ROWS * LANES), KV, 0, 0, tiled=True)
    return slots.reshape(N_KV * ROWS, LANES)


def call(kernel, name, outs, operands, leaving=0, **more):
    kept = len(outs) - leaving
    shapes = [jax.ShapeDtypeStruct(shape, dtype) for shape, dtype in outs[:kept]]
    if leaving:
        shapes += [pltpu.HBM(shape, dtype) for shape, dtype in outs[kept:]]
        specs = [pltpu.VMEM] * kept + [pltpu.HBM] * leaving
        more["out_specs"] = [pl.BlockSpec(memory_space=space) for space in specs]
    params = pltpu.CompilerParams(vmem_limit_bytes=VMEM)
    run = pl.pallas_call(kernel, out_shape=shapes, name=name, compiler_params=params, **more)
    return run(*operands)


def on_device(
    tokens,
    norm_gain,
    w_query,
    w_key,
    w_value,
    w_gate,
    w_forget,
    w_out,
    cache_key,
    cache_value,
    cache_logf,
    lengths,
):
    whole = ((N_KV * ROWS, LANES), F32)
    tile = ((SEQS, LANES), F32)
    small = (tokens, norm_gain[None, :], w_query, w_key, w_value, w_gate, jnp.transpose(w_forget))
    small = small + (jnp.transpose(cache_logf, (0, 2, 1)), lengths[None, :])
    large = [jnp.transpose(cache, (0, 2, 3, 1)) for cache in (cache_key, cache_value)]
    large.append(jnp.transpose(w_out, (0, 2, 1)))
    first, bias, keys, values, w_out = call(
        prep,
        "prep",
        [whole, ((2 * SEQS, SPAN), F32)] + [(x.shape, x.dtype) for x in large],
        [pltpu.with_memory_space_constraint(x, pltpu.HBM) for x in (*small, *large)],
        in_specs=[pl.BlockSpec(memory_space=pltpu.HBM)] * 12,
        scratch_shapes=[pltpu.VMEM(x.shape, x.dtype) for x in small]
        + [pltpu.SemaphoreType.DMA((12,))],
    )
    second, query, sums, shift, logf_new = call(
        attend,
        "attend",
        [whole, tile, tile, ((N_KV, LANES), F32), ((2, SEQS), F32)],
        (exchange(first), keys, values, bias),
        leaving=1,
        scratch_shapes=[pltpu.VMEM((2, SEQS), F32), pltpu.SemaphoreType.DMA],
    )
    heads = (SEQS, 2, HEAD_DIM)
    partial_out, key_new, value_new = call(
        combine,
        "combine",
        [((SEQS, tokens.shape[1]), F32), (heads, jnp.bfloat16), (heads, F32)],
        (exchange(second), query, sums, shift, w_out),
        leaving=2,
        scratch_shapes=[
            pltpu.VMEM(heads, jnp.bfloat16),
            pltpu.VMEM(heads, F32),
            pltpu.SemaphoreType.DMA((2,)),
        ],
    )
    mixed = lax.all_gather(partial_out, "tp").sum(0)
    return mixed, key_new, value_new, jnp.transpose(logf_new)


def solution(mesh):
    finer = Mesh(
        mesh.devices.reshape(mesh.shape["dp"], 8, 8, mesh.shape["tp"]), ("dp", "kv_0", "kv_1", "tp")
    )
    return jax.shard_map(
        on_device,
        mesh=finer,
        in_specs=(
            P("dp", KV),
            P(KV),
            P(KV, "tp", None),
            P(KV, "tp", None),
            P(KV, "tp", None),
            P(KV, "tp", None),
            P(KV, "tp"),
            P("tp", None, KV),
            P("dp", KV, "tp", None),
            P("dp", KV, "tp", None),
            P("dp", KV, "tp"),
            P("dp"),
        ),
        out_specs=(P("dp", KV), P("dp", "tp", None), P("dp", "tp", None), P("dp", "tp")),
        check_vma=False,
    )
```

```python
import jax
import jax.numpy as jnp
from jax import lax
from jax.experimental import pallas as pl
from jax.experimental.pallas import tpu as pltpu
from jax.sharding import Mesh
from jax.sharding import PartitionSpec as P

D = 1024
HEAD_DIM = 64
KV = ("kv_0", "kv_1")
N_KV = 64
SEQS = 8
ROWS = 9
VMEM = 16 * 2**20
SPAN = 512
LANES = 128

eps = 1e-06
very_low = -1e30
HI = lax.Precision.HIGHEST
F32 = jnp.float32
NT = (((1,), (1,)), ((), ()))

FORGET, TOTAL, PIECES, PIECE = 8, 24, 40, 16


def iota(shape, dim):
    return lax.broadcasted_iota(jnp.int32, shape, dim)


def to_row(column, start):
    shape = (SEQS, LANES)
    picked = jnp.where(iota(shape, 1) == iota(shape, 0) + start, column, F32(0.0))
    return jnp.sum(picked, axis=0, keepdims=True)


def to_column(row, start):
    shape = (SEQS, LANES)
    picked = jnp.where(iota(shape, 1) == iota(shape, 0) + start, row, F32(0.0))
    return jnp.sum(picked, axis=1, keepdims=True)


def first_head():
    return iota((SEQS, LANES), 1) < HEAD_DIM


def per_head(values):
    low = jnp.sum(jnp.where(first_head(), values, F32(0.0)), axis=1, keepdims=True)
    high = jnp.sum(jnp.where(first_head(), F32(0.0), values), axis=1, keepdims=True)
    return low, high


def head_norm(values):
    low, high = per_head(values * values)
    return values * lax.rsqrt(jnp.where(first_head(), low, high) * (1.0 / HEAD_DIM) + eps)


def between(start, width):
    lane = iota((SEQS, LANES), 1)
    return (lane >= start) & (lane < start + width)


def rows_at(start):
    return pl.ds(start, SEQS, stride=ROWS)


def fill(slots, values):
    for s in range(SEQS):
        row = jnp.broadcast_to(values[s : s + 1, :], (SEQS, LANES))
        for g in range(N_KV // SEQS):
            slots[rows_at(ROWS * SEQS * g + s), :] = row


def total_row(slots, r):
    parts = [slots[rows_at(ROWS * SEQS * g + r), :] for g in range(N_KV // SEQS)]
    while len(parts) > 1:
        parts = [a + b for a, b in zip(parts[::2], parts[1::2])]
    return jnp.sum(parts[0], axis=0, keepdims=True)


def prep(*refs):
    sources, (slots, bias_out, keys, values, w_out, *local, sems) = refs[:12], refs[12:]
    targets = (*local, keys, values, w_out)
    copies = [
        pltpu.make_async_copy(source, target, sems.at[n])
        for n, (source, target) in enumerate(zip(sources, targets))
    ]
    for copy in copies[:9] + copies[11:] + copies[9:11]:
        copy.start()
    for copy in copies[:9]:
        copy.wait()
    tokens, gain, w_query, w_key, w_value, w_gate, w_forget, logf, lengths = local
    wide = tokens[...].astype(F32)
    squares = jnp.sum(wide * wide, axis=1, keepdims=True)
    scaled = wide * gain[...]

    wide_weights = [w[...].astype(F32) for w in (w_query, w_key, w_value, w_gate)]
    halves = [w[:, h, :] for w in wide_weights for h in range(2)]
    products = jnp.dot(
        scaled, jnp.concatenate(halves, axis=1), precision=HI, preferred_element_type=F32
    )
    forget = lax.dot_general(
        scaled, w_forget[...].astype(F32), NT, precision=HI, preferred_element_type=F32
    )
    shard = lax.axis_index("kv_0") * 8 + lax.axis_index("kv_1")
    limits = jnp.where(iota((SEQS, SEQS), 0) == iota((SEQS, SEQS), 1), lengths[...], 0)
    limits = jnp.sum(limits, axis=1, keepdims=True) - shard * SPAN
    live = iota((SEQS, SPAN), 1) < limits
    shape = (LANES, LANES)
    upper = (iota(shape, 0) > iota(shape, 1)).astype(F32)
    row = to_row(squares, 0)
    blocks = SPAN // LANES
    gates = []
    for h in range(2):
        masked = jnp.where(live, logf[:, h, :], F32(0.0))
        gates += [masked[:, LANES * b : LANES * (b + 1)] for b in range(blocks)]
    inside = jnp.dot(
        jnp.concatenate(gates, axis=0), upper, precision=HI, preferred_element_type=F32
    )
    for h in range(2):
        biases, after = [], jnp.zeros((SEQS, 1), F32)
        for n in reversed(range(blocks * h, blocks * (h + 1))):
            biases.append(inside[SEQS * n : SEQS * (n + 1)] + after)
            after = after + jnp.sum(gates[n], axis=1, keepdims=True)
        bias = jnp.concatenate(biases[::-1], axis=1)
        bias_out[pl.ds(SEQS * h, SEQS), :] = jnp.where(live, bias, F32(very_low))
        row = row + to_row(forget[:, h : h + 1], FORGET + SEQS * h)
        row = row + to_row(after, TOTAL + SEQS * h)
    query, *parts = [products[:, LANES * n : LANES * (n + 1)] for n in range(4)]
    fill(slots, query)
    for c in range(8):
        tail = jnp.broadcast_to(row, (SEQS, LANES))
        for n, part in enumerate(parts):
            start = PIECES + PIECE * n
            moved = pltpu.roll(part, (start - PIECE * c) % LANES, 1)
            tail = jnp.where(between(start, PIECE), moved, tail)
        slots[pl.ds(ROWS * c + SEQS, SEQS, stride=ROWS * 8), :] = tail
    for copy in copies[9:]:
        copy.wait()


def attend(
    slots, cache_key, cache_value, bias, send, query_out, sums_out, shift_out, logf_out, logf_here, sem
):
    seq = iota((SEQS, LANES), 0)
    raw = jnp.zeros((SEQS, LANES), F32)
    for s in range(SEQS):
        raw = jnp.where(seq == s, total_row(slots, s), raw)
    sums = total_row(slots, SEQS)
    inv_root = lax.rsqrt(to_column(sums, 0) * (1.0 / D) + eps)
    query = head_norm(raw * inv_root).astype(jnp.bfloat16)
    query_out[...] = query.astype(F32)
    sums_out[...] = jnp.broadcast_to(sums, (SEQS, LANES))

    logf_row = jnp.zeros((1, LANES), F32)
    for h in range(2):
        forget = to_column(sums, FORGET + SEQS * h) * inv_root
        logf = jnp.minimum(forget, 0.0) - jnp.log1p(jnp.exp(-jnp.abs(forget)))
        logf_here[pl.ds(h, 1), :] = to_row(logf, 0)[:, :SEQS]
        logf_row = logf_row + to_row(logf, TOTAL + SEQS * h)
    copy = pltpu.make_async_copy(logf_here, logf_out, sem)
    copy.start()
    tails = slots[pl.ds(SEQS, N_KV, stride=ROWS), :]
    shape = (N_KV, N_KV)
    upper = (iota(shape, 1) > iota(shape, 0)).astype(F32)
    later = jnp.dot(upper, tails, precision=HI, preferred_element_type=F32)
    shift_out[...] = later + logf_row

    blocks = []
    wide_query = query.astype(F32)
    for s in range(SEQS):
        mine = jnp.where(seq == s, wide_query, F32(0.0))
        low = jnp.where(first_head(), mine, F32(0.0))
        blocks.append(jnp.concatenate([low, mine - low], axis=0))
    spread = jnp.concatenate(blocks, axis=1).astype(jnp.bfloat16)
    keys = cache_key[...].reshape(SEQS * LANES, SPAN)
    scores = jnp.dot(spread, keys, preferred_element_type=F32) * HEAD_DIM ** (-0.5)

    live = bias[...] > F32(0.5 * very_low)
    scores = jnp.where(live, scores + bias[...], F32(very_low))
    peak = jnp.max(scores, axis=1, keepdims=True)
    weights = jnp.where(live, jnp.exp(scores - peak), F32(0.0))
    den = jnp.sum(weights, axis=1, keepdims=True)
    values = cache_value[...].reshape(SEQS * LANES, SPAN)
    crossed = lax.dot_general(
        weights.astype(jnp.bfloat16), values, NT, preferred_element_type=F32
    )
    local = jnp.zeros((SEQS, LANES), F32)
    for s in range(SEQS):
        block = crossed[:, LANES * s : LANES * (s + 1)]
        own = jnp.where(first_head(), block[:SEQS], block[SEQS:])
        local = jnp.where(seq == s, own, local)
    lane = iota((1, LANES), 1)
    row = jnp.where((lane >= PIECES) & (lane < PIECES + 3 * PIECE), sums, F32(0.0))
    for h in range(2):
        rows = slice(SEQS * h, SEQS * (h + 1))
        row = row + to_row(den[rows], SEQS * h) + to_row(peak[rows], TOTAL + SEQS * h)
    tail = jnp.broadcast_to(row, (SEQS, LANES))
    fill(send, local)
    for c in range(8):
        send[pl.ds(ROWS * c + SEQS, SEQS, stride=ROWS * 8), :] = tail
    copy.wait()


def combine(
    slots, query, sums, shift, w_out, partial_out, key_out, value_out, key_here, value_here, sems
):
    sums_row = sums[0:1, :]
    inv_root = lax.rsqrt(to_column(sums_row, 0) * (1.0 / D) + eps)
    parts = [jnp.zeros((SEQS, LANES), F32) for _ in range(3)]
    for c in range(8):
        tail = slots[pl.ds(ROWS * c + SEQS, SEQS, stride=ROWS * 8), :]
        for n in range(3):
            start = PIECES + PIECE * n
            moved = pltpu.roll(tail, (PIECE * c - start) % LANES, 1)
            parts[n] = jnp.where(between(PIECE * c, PIECE), moved, parts[n])
    key, value, gate = (part * inv_root for part in parts)
    key = head_norm(key).astype(jnp.bfloat16)
    for h in range(2):
        part = slice(HEAD_DIM * h, HEAD_DIM * (h + 1))
        key_here[:, h, :] = key[:, part]
        value_here[:, h, :] = value[:, part]
    copies = [
        pltpu.make_async_copy(key_here, key_out, sems.at[0]),
        pltpu.make_async_copy(value_here, value_out, sems.at[1]),
    ]
    for copy in copies:
        copy.start()
    score_new = [x * HEAD_DIM ** (-0.5) for x in per_head(query[...] * key.astype(F32))]
    tails = slots[pl.ds(SEQS, N_KV, stride=ROWS), :]
    score_row = jnp.zeros((1, LANES), F32)
    for h in range(2):
        score_row = score_row + to_row(score_new[h], TOTAL + SEQS * h)
    peaks = tails + shift[...]
    peak = jnp.maximum(jnp.max(peaks, axis=0, keepdims=True), score_row)
    lane = iota((N_KV, LANES), 1)
    stats = (lane >= TOTAL) & (lane < TOTAL + 2 * SEQS)
    factors = jnp.where(stats, jnp.exp(jnp.where(stats, peaks - peak, F32(0.0))), F32(0.0))
    weight_new = jnp.exp(jnp.where(stats[0:1], score_row - peak, F32(0.0)))
    den = jnp.sum(factors * pltpu.roll(tails, TOTAL, 1), axis=0, keepdims=True) + weight_new
    low, seq = first_head(), iota((SEQS, LANES), 0)
    weighted = jnp.zeros((SEQS, LANES), F32)
    for s in range(SEQS):
        sums_of = []
        for g in range(N_KV // SEQS):
            own = factors[SEQS * g : SEQS * (g + 1)]
            first, second = (own[:, n : n + 1] for n in (TOTAL + s, TOTAL + SEQS + s))
            sums_of.append(jnp.where(low, first, second) * slots[rows_at(ROWS * SEQS * g + s), :])
        while len(sums_of) > 1:
            sums_of = [a + b for a, b in zip(sums_of[::2], sums_of[1::2])]
        weighted = jnp.where(seq == s, jnp.sum(sums_of[0], axis=0, keepdims=True), weighted)

    def lanes_of(row):
        return jnp.where(low, to_column(row, TOTAL), to_column(row, TOTAL + SEQS))

    attended = (weighted + lanes_of(weight_new) * value) / lanes_of(den)
    silu = gate / (1.0 + jnp.exp(-gate))
    gated = (head_norm(attended) * silu).astype(jnp.bfloat16)
    mixed = jnp.zeros((SEQS, w_out.shape[1]), F32)
    for h in range(2):
        half = gated[:, HEAD_DIM * h : HEAD_DIM * (h + 1)]
        mixed = mixed + lax.dot_general(half, w_out[h], NT, preferred_element_type=F32)
    partial_out[...] = mixed
    for copy in copies:
        copy.wait()


def exchange(slots):
    slots = lax.all_to_all(slots.reshape(N_KV, 1, ROWS * LANES), KV, 0, 0, tiled=True)
    return slots.reshape(N_KV * ROWS, LANES)


def call(kernel, name, outs, operands, leaving=0, **more):
    kept = len(outs) - leaving
    shapes = [jax.ShapeDtypeStruct(shape, dtype) for shape, dtype in outs[:kept]]
    if leaving:
        shapes += [pltpu.HBM(shape, dtype) for shape, dtype in outs[kept:]]
        specs = [pltpu.VMEM] * kept + [pltpu.HBM] * leaving
        more["out_specs"] = [pl.BlockSpec(memory_space=space) for space in specs]
    params = pltpu.CompilerParams(vmem_limit_bytes=VMEM)
    run = pl.pallas_call(kernel, out_shape=shapes, name=name, compiler_params=params, **more)
    return run(*operands)


def on_device(
    tokens,
    norm_gain,
    w_query,
    w_key,
    w_value,
    w_gate,
    w_forget,
    w_out,
    cache_key,
    cache_value,
    cache_logf,
    lengths,
):
    whole = ((N_KV * ROWS, LANES), F32)
    tile = ((SEQS, LANES), F32)
    small = (tokens, norm_gain[None, :], w_query, w_key, w_value, w_gate, jnp.transpose(w_forget))
    small = small + (jnp.transpose(cache_logf, (0, 2, 1)), lengths[None, :])
    large = [jnp.transpose(cache, (0, 2, 3, 1)) for cache in (cache_key, cache_value)]
    large.append(jnp.transpose(w_out, (0, 2, 1)))
    first, bias, keys, values, w_out = call(
        prep,
        "prep",
        [whole, ((2 * SEQS, SPAN), F32)] + [(x.shape, x.dtype) for x in large],
        [pltpu.with_memory_space_constraint(x, pltpu.HBM) for x in (*small, *large)],
        in_specs=[pl.BlockSpec(memory_space=pltpu.HBM)] * 12,
        scratch_shapes=[pltpu.VMEM(x.shape, x.dtype) for x in small]
        + [pltpu.SemaphoreType.DMA((12,))],
    )
    second, query, sums, shift, logf_new = call(
        attend,
        "attend",
        [whole, tile, tile, ((N_KV, LANES), F32), ((2, SEQS), F32)],
        (exchange(first), keys, values, bias),
        leaving=1,
        scratch_shapes=[pltpu.VMEM((2, SEQS), F32), pltpu.SemaphoreType.DMA],
    )
    heads = (SEQS, 2, HEAD_DIM)
    partial_out, key_new, value_new = call(
        combine,
        "combine",
        [((SEQS, tokens.shape[1]), F32), (heads, jnp.bfloat16), (heads, F32)],
        (exchange(second), query, sums, shift, w_out),
        leaving=2,
        scratch_shapes=[
            pltpu.VMEM(heads, jnp.bfloat16),
            pltpu.VMEM(heads, F32),
            pltpu.SemaphoreType.DMA((2,)),
        ],
    )
    mixed = lax.all_gather(partial_out, "tp").sum(0)
    return mixed, key_new, value_new, jnp.transpose(logf_new)


def solution(mesh):
    finer = Mesh(
        mesh.devices.reshape(mesh.shape["dp"], 8, 8, mesh.shape["tp"]), ("dp", "kv_0", "kv_1", "tp")
    )
    return jax.shard_map(
        on_device,
        mesh=finer,
        in_specs=(
            P("dp", KV),
            P(KV),
            P(KV, "tp", None),
            P(KV, "tp", None),
            P(KV, "tp", None),
            P(KV, "tp", None),
            P(KV, "tp"),
            P("tp", None, KV),
            P("dp", KV, "tp", None),
            P("dp", KV, "tp", None),
            P("dp", KV, "tp"),
            P("dp"),
        ),
        out_specs=(P("dp", KV), P("dp", "tp", None), P("dp", "tp", None), P("dp", "tp")),
        check_vma=False,
    )
```
